128 devices in a mesh: sp: 16 (over z, y), fs: 4 (over x), tp: 2 (over core).
Axes of the slice: x: 4, y: 4, z: 4, core: 2. Of those that a mesh axis runs over, the one named last changes fastest.
Arguments:
- tokens: bfloat16 [8, 6144, 2048], P('fs', ('sp', 'tp')), may hold values from -6 to 6
- norm_gain: float32 [2048], replicated, may hold values from 0.1 to 1.9
- chain_entry: bfloat16 [2048, 2048], P(('sp', 'fs'), 'tp'), may hold values from -0.125 to 0.125
- pool_entry: bfloat16 [2048, 2048], P(('sp', 'fs'), 'tp'), may hold values from -0.125 to 0.125
- conv_taps: bfloat16 [4, 2048], P(None, 'tp'), may hold values from -3 to 3
- recur_gate: bfloat16 [8, 256, 256], P('tp'), may hold values from -0.375 to 0.375
- input_gate: bfloat16 [8, 256, 256], P('tp'), may hold values from -0.375 to 0.375
- decay_log: float32 [2048], P('tp'), may hold values from -9 to 5
- decay_shift: float32 [8, 6144, 2048], P('fs', 'sp', 'tp'), may hold values from -1 to 0
- start_state: float32 [8, 2048], P('fs', 'tp'), may hold values from -6 to 6
- pool_mix: bfloat16 [8, 256, 256], P('tp'), may hold values from -0.375 to 0.375
- pool_scale: float32 [2048], P('tp'), may hold values from 0.1 to 1.9
- chain_exit: bfloat16 [2048, 2048], P('tp', ('sp', 'fs')), may hold values from -0.09375 to 0.09375
- pool_exit: bfloat16 [2048, 2048], P('tp', ('sp', 'fs')), may hold values from -0.09375 to 0.09375
Outputs:
- mixed_rows: bfloat16 [8, 6144, 2048], P('fs', ('sp', 'tp'))
The draws below stay inside these ranges and needn't reach their ends.
All inputs are finite; a program needn't handle non-finite values.
Results may differ from the reference program's by a relative error of at most 0.01.
Values may be sent and summed in bfloat16 or wider, within the bound.
A program may use at most 128 MiB of HBM per device.

```python
import math
import jax
import jax.numpy as jnp
from jax import lax

D = 2048
HEAD = 256
CHAIN_HEADS = 8
POOL_GROUPS = 8
CONV_TAPS = 4
POOL_SPAN = 16
TOK_DEV = 384
CHAIN_WIDTH = 2048
POOL_WIDTH = 2048
LEN = 6144
SEQS = 8


def draw_decay_log(key, part):
    inner = jax.random.fold_in(key, 7)
    return jax.random.uniform(inner, (CHAIN_WIDTH,), jnp.float32, -9.0, 5.0)


def draw_decay_shift(key, part):
    inner = jax.random.fold_in(key, 11)
    first_key, second_key, third_key, fourth_key, fifth_key, sixth_key, seventh_key = jax.random.split(inner, 7)
    block_span = TOK_DEV // 4
    block_total = SEQS * LEN // block_span
    slowness = jnp.exp(jax.random.uniform(first_key, (block_total, 1, CHAIN_WIDTH), jnp.float32, math.log(0.1), math.log(0.8)))
    jitter = jax.random.uniform(second_key, (block_total, block_span, CHAIN_WIDTH), jnp.float32, 0.5, 1.5)
    fast_share = 0.5
    fast_pick = jax.random.uniform(fifth_key, (CHAIN_WIDTH,), jnp.float32) < fast_share
    fast_rate = jnp.exp(jax.random.uniform(sixth_key, (CHAIN_WIDTH,), jnp.float32, math.log(0.012), math.log(0.035)))
    fast_boost = jnp.exp(jax.random.uniform(seventh_key, (block_total, 1, CHAIN_WIDTH), jnp.float32, math.log(0.6), math.log(1.6)))
    rate = slowness / LEN + jnp.where(fast_pick, fast_rate, 0.0)[None, None, :] * fast_boost
    steady = -(rate * jitter).reshape(SEQS, LEN, CHAIN_WIDTH)
    places = jax.random.randint(third_key, (SEQS, 4), 0, LEN)
    struck = jnp.any(jnp.arange(LEN)[None, :, None] == places[:, None, :], axis=2)
    depth = jax.random.uniform(fourth_key, (SEQS, LEN, CHAIN_WIDTH), jnp.float32, -0.7, -0.2)
    return steady + jnp.where(struck[:, :, None], depth, 0.0)


def steps_of(stream_key, extent, pieces, least, high):
    level, own = 1.0, jax.random.fold_in(stream_key, 6)
    for dim, shards_of in pieces:
        heights = jnp.exp(jax.random.uniform(jax.random.fold_in(own, dim), (shards_of,), jnp.float32, least / len(pieces), high / len(pieces)))
        level = level * jnp.repeat(heights, extent[dim] // shards_of).reshape([-1 if axis == dim else 1 for axis in range(len(extent))])
    return level


def scatter_about(stream_key, dims, width, reach, pieces=(), kind=jnp.bfloat16):
    array = width * jax.random.normal(stream_key, dims, jnp.float32)
    if pieces:
        array = array * steps_of(stream_key, dims, pieces, -0.22, 0.18)
    return jnp.clip(array, -reach, reach).astype(kind)


def setup_inputs(seed: int = 0) -> dict:
    seeds = jax.random.split(jax.random.key(seed), 15)
    return {
        "tokens": scatter_about(seeds[0], (SEQS, LEN, D), 1.0, 6.0, ((0, 4), (1, 32))),
        "norm_gain": jnp.clip(1.0 + 0.18 * jax.random.normal(seeds[1], (D,), jnp.float32), 0.1, 1.9),
        "chain_entry": scatter_about(seeds[2], (D, CHAIN_WIDTH), D ** -0.5, 0.125, ((0, 64), (1, 2))),
        "pool_entry": scatter_about(seeds[3], (D, POOL_WIDTH), D ** -0.5, 0.125, ((0, 64), (1, 2))),
        "conv_taps": scatter_about(seeds[4], (CONV_TAPS, CHAIN_WIDTH), CONV_TAPS ** -0.5, 3.0, ((1, 2),)),
        "recur_gate": scatter_about(seeds[5], (CHAIN_HEADS, HEAD, HEAD), HEAD ** -0.5, 0.375, ((0, 2),)),
        "input_gate": scatter_about(seeds[6], (CHAIN_HEADS, HEAD, HEAD), HEAD ** -0.5, 0.375, ((0, 2),)),
        "decay_log": draw_decay_log(jax.random.fold_in(seeds[14], 71), 0),
        "decay_shift": draw_decay_shift(jax.random.fold_in(seeds[14], 71), 0),
        "start_state": scatter_about(seeds[9], (SEQS, CHAIN_WIDTH), 1.0, 6.0, ((0, 4), (1, 2)), jnp.float32),
        "pool_mix": scatter_about(seeds[10], (POOL_GROUPS, HEAD, HEAD), HEAD ** -0.5, 0.375, ((0, 2),)),
        "pool_scale": jnp.clip(1.0 + 0.18 * jax.random.normal(seeds[11], (POOL_WIDTH,), jnp.float32), 0.1, 1.9),
        "chain_exit": scatter_about(seeds[12], (CHAIN_WIDTH, D), (CHAIN_WIDTH + POOL_WIDTH) ** -0.5, 0.09375, ((0, 2), (1, 64))),
        "pool_exit": scatter_about(seeds[13], (POOL_WIDTH, D), (CHAIN_WIDTH + POOL_WIDTH) ** -0.5, 0.09375, ((0, 2), (1, 64))),
    }


NORM_EPSILON = 1e-06
RECUR_SCALE = 8.0

def block_map(values, weight):
    row_total = values.shape[0]
    groups, block_width, _ = weight.shape
    blocks = values.astype(jnp.float32).reshape(row_total, groups, block_width)
    mapped = jnp.einsum('sgi,gij->sgj', blocks, weight.astype(jnp.float32))
    return mapped.reshape(row_total, groups * block_width)

def combine(earlier, latter):
    return (earlier[0] * latter[0], latter[0] * earlier[1] + latter[1])

def trailing(padded, row_total, window_id):
    sum_two = padded[1:] + padded[:-1]
    sum_four = sum_two[2:] + sum_two[:-2]
    sum_eight = sum_four[4:] + sum_four[:-4]
    sixteen = sum_eight[8:] + sum_eight[:-8]
    return jnp.where(window_id == 0, sum_two[-row_total:], jnp.where(window_id == 1, sum_four[-row_total:], jnp.where(window_id == 2, sum_eight[-row_total:], sixteen[-row_total:])))

def reference(tokens, norm_gain, chain_entry, pool_entry, conv_taps, recur_gate, input_gate, decay_log, decay_shift, start_state, pool_mix, pool_scale, chain_exit, pool_exit):
    channel = jnp.arange(POOL_WIDTH, dtype=jnp.int32) // HEAD
    window_id = (channel % 4)[None, :]
    window = jnp.power(2.0, (window_id + 1).astype(jnp.float32))
    position = jnp.arange(LEN, dtype=jnp.float32)[:, None]
    counts = jnp.minimum(position + 1.0, window)
    decay_rate = jnp.exp(decay_log) / LEN

    def one_sequence(inputs):
        values, shift_rows, begin_state = inputs
        widened = values.astype(jnp.float32)
        normed = (widened * lax.rsqrt(lax.optimization_barrier(jnp.mean(widened * widened, axis=-1, keepdims=True)) + NORM_EPSILON) * norm_gain.astype(jnp.float32)).astype(jnp.bfloat16)
        chain_input = jnp.dot(normed, chain_entry, preferred_element_type=jnp.float32).astype(jnp.bfloat16)
        pool_input = jnp.dot(normed, pool_entry, preferred_element_type=jnp.float32).astype(jnp.bfloat16)
        padded = jnp.pad(chain_input.astype(jnp.float32), ((CONV_TAPS - 1, 0), (0, 0)))
        conv_out = jnp.zeros((LEN, CHAIN_WIDTH), jnp.float32)
        for offset in range(CONV_TAPS):
            conv_out = conv_out + padded[offset:offset + LEN] * conv_taps[offset].astype(jnp.float32)
        conv_out = conv_out.astype(jnp.bfloat16)
        gate_recur = jax.nn.sigmoid(block_map(conv_out, recur_gate))
        gate_input = jax.nn.sigmoid(block_map(conv_out, input_gate))
        log_decay = -RECUR_SCALE * gate_recur * decay_rate + shift_rows
        decay_factor = jnp.exp(log_decay)
        drive_term = jnp.sqrt(-jnp.expm1(2.0 * log_decay)) * gate_input * conv_out.astype(jnp.float32)
        drive_term = drive_term.at[0].add(decay_factor[0] * begin_state)
        state = lax.associative_scan(combine, (decay_factor, drive_term), axis=0)[1]
        recurrent = state.astype(jnp.bfloat16)
        pool_pad = jnp.pad(pool_input.astype(jnp.float32), ((POOL_SPAN - 1, 0), (0, 0)))
        trail_sum = trailing(pool_pad, LEN, window_id)
        pool_diff = (trail_sum / counts - pool_input.astype(jnp.float32)).astype(jnp.bfloat16)
        pooled = (block_map(pool_diff, pool_mix) * pool_scale.astype(jnp.float32)).astype(jnp.bfloat16)
        mixed_rows = jnp.dot(recurrent, chain_exit, preferred_element_type=jnp.float32) + jnp.dot(pooled, pool_exit, preferred_element_type=jnp.float32)
        return mixed_rows.astype(jnp.bfloat16)
    return lax.map(one_sequence, (tokens, decay_shift, start_state))
```

```python
import jax
import jax.numpy as jnp
from jax import lax
from jax.experimental import pallas as pl
from jax.experimental.pallas import tpu as pltpu
from jax.sharding import PartitionSpec as P

MESH = pl.DeviceIdType.MESH
NORM_EPSILON = 1e-06
RECUR_SCALE = 8.0
HALO = 16
ROWS = 384
HALF = ROWS // 2
HEAD = 256
HEADS = 4
WIDTH = HEADS * HEAD
D = 2048
SEQ = 2
CHUNK = 128
STRIP = 32
ALL = slice(None)
F32 = jnp.float32
BF16 = jnp.bfloat16

ORDERS = ("xyz", "yzx", "zxy")
ARRAYS = (
    (0, ((0, 384), (384, 384), (768, 256))),
    (0, ((1024, 256), (1280, 384), (1664, 384))),
    (1, ((0, 384), (384, 256), (640, 384))),
    (1, ((1024, 384), (1408, 384), (1792, 256))),
)
MESSAGES = 24


def minus_expm1(v):
    series = v * (1.0 / 5040.0) + (1.0 / 720.0)
    for c in (1.0 / 120.0, 1.0 / 24.0, 1.0 / 6.0, 0.5, 1.0):
        series = series * v + c
    return jnp.where(v > -0.35, -v * series, 1.0 - jnp.exp(v))


def sigmoid(v):
    return 0.5 * jnp.tanh(0.5 * v) + 0.5


def kernel(
    tok_in, gain_ref, e_in, f_in, taps_ref, rgate_in, igate_in, dlog_ref, shift_in, start_ref,
    mix_in, scale_ref,
    out_ref,
    E, F, X, N, CP, A, B, G, rgate, igate, mix, R, CS, CR, OUTS, OUTR, OUTV,
    ssem, rsem, lsem, xsem, csend, crecv, osend, orecv, vsem,
):
    sp = lax.axis_index("sp")
    x = lax.axis_index("fs")
    c = lax.axis_index("tp")
    z = sp // 4
    y = sp % 4
    at = dict(x=x, y=y, z=z)
    after = lax.rem(sp + 1, 16)
    before = lax.rem(sp + 15, 16)

    place = {(d, by): lax.rem(at[d] + by + 4, 4) for d in "xyz" for by in (-1, 0, 1, 2)}

    def off(dim, by):
        return place[dim, by]

    def near(dim, by):
        p = dict(at)
        p[dim] = off(dim, by)
        return (p["z"] * 4 + p["y"], p["x"], c)

    own_rows = pl.ds(pl.multiple_of(HALO + c * HALF, 16), HALF)
    local = [
        pltpu.make_async_copy(src, dst, lsem.at[k])
        for k, (src, dst) in enumerate(
            (
                (e_in, E.at[z, y, x]),
                (tok_in, X.at[:, own_rows]),
                (f_in, F.at[z, y, x]),
                (shift_in, A),
                (rgate_in, rgate),
                (igate_in, igate),
                (mix_in, mix),
            )
        )
    ]
    for cp in local:
        cp.start()

    barrier = pltpu.get_barrier_semaphore()

    def greet(device):
        pl.semaphore_signal(barrier, inc=1, device_id=device, device_id_type=MESH)

    for by in (-1, 1):
        greet(near("x", by))
    greet((sp, x, 1 - c))
    for k in range(1, 16):
        greet((lax.rem(sp + k, 16), x, c))
    pl.semaphore_wait(barrier, 18)

    sent = []
    W = (E, F)

    def message(a, r, k, where, half, dim, by):
        buf, thirds = ARRAYS[a]
        lanes = pl.ds(*thirds[r])
        rows = (ALL, pl.ds(0, 16), pl.ds(16, 16))[half]
        v = W[buf].at[tuple(ALL if where[d] is None else where[d] for d in "zyx") + (rows, lanes)]
        return pltpu.make_async_remote_copy(
            src_ref=v, dst_ref=v, send_sem=ssem.at[a, r, k], recv_sem=rsem.at[a, r, k],
            device_id=near(dim, by), device_id_type=MESH,
        )

    def send(*args):
        cp = message(*args)
        cp.start()
        sent.append(args)

    def exchange(a, r, base, where, dim):
        for j, by in ((0, 1), (1, -1)):
            send(a, r, base + j, where, 0, dim, by)

    def shifted(where, dim, by):
        w = dict(where)
        w[dim] = off(dim, by)
        return w

    def pass_on(a, r, base, where, dim, side):
        w = shifted(where, dim, side)
        j = 0 if side == -1 else 1
        message(a, r, base + j, w, 0, dim, 1).wait_recv()
        send(a, r, base + 2 + j, w, 1 + j, dim, -side)

    def halves(a, r, base, where, dim):
        w = shifted(where, dim, 2)
        message(a, r, base + 2, w, 1, dim, 1).wait_recv()
        message(a, r, base + 3, w, 2, dim, 1).wait_recv()

    def w1(r):
        return dict(at)

    def w2(r):
        w = dict(at)
        w[ORDERS[r][0]] = None
        return w

    def w3(r, g):
        w = w2(r)
        w[ORDERS[r][1]] = off(ORDERS[r][1], (0, -1, 1, 2)[g])
        return w

    thirds = range(3)

    def s0(a):
        for r in thirds:
            exchange(a, r, 0, w1(r), ORDERS[r][0])

    def s1(a, side):
        for r in thirds:
            pass_on(a, r, 0, w1(r), ORDERS[r][0], side)

    def s2(a):
        for r in thirds:
            halves(a, r, 0, w1(r), ORDERS[r][0])
            exchange(a, r, 4, w2(r), ORDERS[r][1])
        for r in thirds:
            exchange(a, r, 8, w3(r, 0), ORDERS[r][2])

    def s3(a, side, g):
        for r in thirds:
            pass_on(a, r, 4, w2(r), ORDERS[r][1], side)
            exchange(a, r, 8 + 4 * g, w3(r, g), ORDERS[r][2])

    def s4(a, g, side):
        for r in thirds:
            pass_on(a, r, 8 + 4 * g, w3(r, g), ORDERS[r][2], side)

    def s5(a):
        for r in thirds:
            halves(a, r, 4, w2(r), ORDERS[r][1])
            exchange(a, r, 20, w3(r, 3), ORDERS[r][2])

    def s6(a):
        for g in range(4):
            for r in thirds:
                halves(a, r, 8 + 4 * g, w3(r, g), ORDERS[r][2])

    def stages(a):
        more = a + 1 < len(ARRAYS)
        steps = []
        if more:
            steps.append(lambda: s0(a + 1))
        steps.append(lambda: s3(a, -1, 1))
        steps.append(lambda: s3(a, 1, 2))
        if more:
            steps.append(lambda: s1(a + 1, -1))
            steps.append(lambda: s1(a + 1, 1))
        steps.append(lambda: s4(a, 0, -1))
        steps.append(lambda: s4(a, 0, 1))
        steps.append(lambda: s5(a))
        steps.append(lambda: s4(a, 1, -1))
        steps.append(lambda: s4(a, 1, 1))
        steps.append(lambda: s4(a, 2, -1))
        steps.append(lambda: s4(a, 2, 1))
        if more:
            steps.append(lambda: s2(a + 1))
        steps.append(lambda: s4(a, 3, -1))
        steps.append(lambda: s4(a, 3, 1))
        steps.append(lambda: s6(a))
        return steps

    def beside(steps, total, body):
        def one(i, carry):
            body(i)
            for k, step in enumerate(steps):
                pl.when(i == (k * total) // len(steps))(step)
            return carry
        lax.fori_loop(0, total, one, 0)

    local[0].wait()
    s0(0)
    local[1].wait()
    tok_copy = pltpu.make_async_remote_copy(
        src_ref=X.at[:, own_rows], dst_ref=X.at[:, own_rows], send_sem=xsem.at[0],
        recv_sem=xsem.at[1], device_id=(sp, x, 1 - c), device_id_type=MESH,
    )
    tok_copy.start()
    s1(0, -1)
    s1(0, 1)
    s2(0)
    other_rows = pl.ds(pl.multiple_of(HALO + (1 - c) * HALF, 16), HALF)
    pltpu.make_async_remote_copy(
        src_ref=X.at[:, other_rows], dst_ref=X.at[:, other_rows], send_sem=xsem.at[0],
        recv_sem=xsem.at[1], device_id=(sp, x, 1 - c), device_id_type=MESH,
    ).wait_recv()
    halo_copy = pltpu.make_async_remote_copy(
        src_ref=X.at[:, pl.ds(ROWS, HALO)], dst_ref=X.at[:, pl.ds(0, HALO)], send_sem=xsem.at[2],
        recv_sem=xsem.at[3], device_id=(after, x, c), device_id_type=MESH,
    )
    halo_copy.start()
    for k in range(2, 7):
        local[k].wait()

    first = jnp.where(sp == 0, 0.0, 1.0).astype(F32)

    def norm_tile(s, row, factor):
        v = X[s, pl.ds(row, 16), :].astype(F32)
        r = lax.rsqrt(jnp.mean(v * v, axis=-1, keepdims=True) + NORM_EPSILON)
        if factor is not None:
            r = r * factor
        N[s, pl.ds(row, 16), :] = (v * r * gain_ref[...]).astype(BF16)

    def norm_body(i):
        s = i // 24
        norm_tile(s, pl.multiple_of(HALO + (i % 24) * 16, 16), None)

    early = stages(0)
    early[0]()
    early[1]()
    early[2]()
    lax.fori_loop(0, 48, lambda i, q: (norm_body(i), q)[1], 0)
    for step in early[3:6]:
        step()
    halo_copy.wait_recv()
    for s in range(SEQ):
        norm_tile(s, 0, first)
    for step in early[6:]:
        step()

    def entry_tile(s, col):
        cols = pl.ds(col, HEAD)
        w = E[:, :, :, :, cols].reshape(D, HEAD)
        acc = jnp.dot(N[s], w, preferred_element_type=F32)
        CP[s, :, cols] = acc.astype(BF16).astype(F32)

    def entry_body(base):
        def body(i):
            entry_tile(i % 2, pl.multiple_of(base + (i // 2) * HEAD, HEAD))
        return body

    sub = lax.broadcasted_iota(jnp.int32, (STRIP, HEAD), 0) % 8

    def gates_body(i):
        h = i // 6
        s = (i // 3) % 2
        row = pl.multiple_of((i % 3) * CHUNK, CHUNK)
        cols = pl.ds(pl.multiple_of(h * HEAD, HEAD), HEAD)
        v = CP[s, pl.ds(row, CHUNK + HALO), cols]
        conv = pltpu.roll(v, 3, 0) * taps_ref[0:1, cols]
        conv = conv + pltpu.roll(v, 2, 0) * taps_ref[1:2, cols]
        conv = conv + pltpu.roll(v, 1, 0) * taps_ref[2:3, cols]
        conv = conv + v * taps_ref[3:4, cols]
        conv = conv[HALO:].astype(BF16)
        G[0] = jnp.dot(conv, rgate[h], preferred_element_type=F32)
        G[1] = jnp.dot(conv, igate[h], preferred_element_type=F32)
        G[2] = conv.astype(F32)
        rate = jnp.exp(dlog_ref[:, cols]) * (-RECUR_SCALE / 6144.0)
        for k in range(CHUNK // STRIP):
            rows = pl.ds(k * STRIP, STRIP)
            to = pl.ds(pl.multiple_of(row + k * STRIP, STRIP), STRIP)
            log_decay = sigmoid(G[0, rows]) * rate + A[s, to, cols]
            a = jnp.exp(log_decay)
            b = jnp.sqrt(minus_expm1(2.0 * log_decay)) * sigmoid(G[1, rows]) * G[2, rows]
            for d in (1, 2, 4):
                keep = sub >= d
                up_a = jnp.where(keep, pltpu.roll(a, d, 0), 1.0)
                up_b = jnp.where(keep, pltpu.roll(b, d, 0), 0.0)
                b = a * up_b + b
                a = a * up_a
            A[s, to, cols] = a
            B[s, to, cols] = b

    def scan_step(t, carry):
        out = []
        rows = pl.ds(pl.multiple_of(t * 8, 8), 8)
        for s in range(SEQ):
            ha, hb = carry[2 * s], carry[2 * s + 1]
            a, b = A[s, rows, :], B[s, rows, :]
            b = a * hb + b
            a = a * ha
            A[s, rows, :] = a
            B[s, rows, :] = b
            out.append(jnp.broadcast_to(a[7:8], (8, WIDTH)))
            out.append(jnp.broadcast_to(b[7:8], (8, WIDTH)))
        return tuple(out)

    def pool_group(g, i):
        w = 2 ** (g + 1)
        s = i // 3
        row = pl.multiple_of((i % 3) * CHUNK, CHUNK)
        cols = pl.ds(WIDTH + g * HEAD, HEAD)
        v = CP[s, pl.ds(row, CHUNK + HALO), cols]
        total = v
        for d in range(g + 1):
            total = total + pltpu.roll(total, 2 ** d, 0)
        position = (sp * ROWS + row + lax.broadcasted_iota(jnp.int32, (CHUNK, HEAD), 0)).astype(F32)
        share = 1.0 / jnp.minimum(position + 1.0, float(w))
        diff = (total[HALO:] * share - v[HALO:]).astype(BF16)
        mixed = jnp.dot(diff, mix[g], preferred_element_type=F32)
        R[s, pl.ds(row, CHUNK), cols] = (mixed * scale_ref[:, pl.ds(g * HEAD, HEAD)]).astype(BF16)

    def pool_body(i):
        for g in range(HEADS):
            pool_group(g, i)

    steps = stages(1)
    beside(steps[:6], 8, entry_body(0))
    beside(steps[6:], 24, gates_body)
    one = jnp.ones((8, WIDTH), F32)
    nought = jnp.zeros((8, WIDTH), F32)
    ends = lax.fori_loop(0, ROWS // 8, scan_step, (one, nought, one, nought))
    for s in range(SEQ):
        CS[pl.ds(s, 1), :] = ends[2 * s][0:1]
        CS[pl.ds(2 + s, 1), :] = ends[2 * s + 1][0:1]
    steps = stages(2)
    steps[0]()
    steps[1]()

    def carry_to(k):
        return pltpu.make_async_remote_copy(
            src_ref=CS, dst_ref=CR.at[sp], send_sem=csend.at[k], recv_sem=crecv.at[sp],
            device_id=(lax.rem(sp + k, 16), x, c), device_id_type=MESH,
        )

    def carry_from(j):
        return pltpu.make_async_remote_copy(
            src_ref=CS, dst_ref=CR.at[j], send_sem=csend.at[0], recv_sem=crecv.at[j],
            device_id=(j, x, c), device_id_type=MESH,
        )

    for k in range(1, 16):
        carry_to(k).start()
    beside(steps[2:9], 8, entry_body(WIDTH))
    beside(steps[9:14], 6, pool_body)
    for k in range(1, 16):
        carry_from(lax.rem(sp + 16 - k, 16)).wait_recv()
    h = start_ref[...]
    for j in range(15):
        h = jnp.where(j < sp, CR[j, 0:2, :] * h + CR[j, 2:4, :], h)

    def state_body(i):
        rows = pl.ds(pl.multiple_of(i * STRIP, STRIP), STRIP)
        for s in range(SEQ):
            R[s, rows, pl.ds(0, WIDTH)] = (A[s, rows, :] * h[s:s + 1] + B[s, rows, :]).astype(BF16)

    lax.fori_loop(0, ROWS // STRIP, lambda i, q: (state_body(i), q)[1], 0)
    for step in steps[14:]:
        step()

    mine = pl.ds(pl.multiple_of(c * HALF, 16), HALF)
    theirs = pl.ds(pl.multiple_of((1 - c) * HALF, 16), HALF)
    NT = (((1,), (1,)), ((), ()))

    def exit_weights(t, k0):
        return F[t // 2, pl.ds(2 * (t % 2), 2), :, :, pl.ds(k0, WIDTH)].reshape(HEAD, WIDTH)

    def chain_exit_body(t):
        cols = pl.ds(pl.multiple_of(t * HEAD, HEAD), HEAD)
        w = exit_weights(t, 0)
        for s in range(SEQ):
            CP[s, pl.ds(0, ROWS), cols] = lax.dot_general(
                R[s, :, pl.ds(0, WIDTH)], w, NT, preferred_element_type=F32
            )

    beside(stages(3), 8, chain_exit_body)

    def out_copy(t):
        cols = pl.ds(pl.multiple_of(t * HEAD, HEAD), HEAD)
        return pltpu.make_async_remote_copy(
            src_ref=OUTS.at[:, :, cols], dst_ref=OUTR.at[:, :, cols], send_sem=osend.at[t],
            recv_sem=orecv.at[t], device_id=(sp, x, 1 - c), device_id_type=MESH,
        )

    def write_out(t):
        cols = pl.ds(pl.multiple_of(t * HEAD, HEAD), HEAD)
        return pltpu.make_async_copy(OUTV.at[:, :, cols], out_ref.at[:, :, cols], vsem.at[t])

    def pool_exit_body(t):
        cols = pl.ds(pl.multiple_of(t * HEAD, HEAD), HEAD)
        w = exit_weights(t, WIDTH)
        for s in range(SEQ):
            OUTS[s, :, cols] = (
                lax.dot_general(
                    R[s, theirs, pl.ds(WIDTH, WIDTH)], w, NT, preferred_element_type=F32
                )
                + CP[s, theirs, cols]
            ).astype(BF16)
        for s in range(SEQ):
            CP[s, mine, cols] += lax.dot_general(
                R[s, mine, pl.ds(WIDTH, WIDTH)], w, NT, preferred_element_type=F32
            )
        out_copy(t).start()

    def finish(t):
        cols = pl.ds(pl.multiple_of(t * HEAD, HEAD), HEAD)
        out_copy(t).wait_recv()
        for s in range(SEQ):
            OUTV[s, :, cols] = (CP[s, mine, cols] + OUTR[s, :, cols].astype(F32)).astype(BF16)
        write_out(t).start()

    def last_body(t, q):
        pool_exit_body(t)

        @pl.when(t >= 3)
        def _():
            finish(t - 3)
        return q

    lax.fori_loop(0, 8, last_body, 0)
    for t in range(5, 8):
        finish(t)

    for args in sent:
        message(*args).wait_send()
    tok_copy.wait_send()
    halo_copy.wait_send()
    for k in range(1, 16):
        carry_to(k).wait_send()
    for t in range(8):
        out_copy(t).wait_send()
        write_out(t).wait()


def per_device(
    tokens, norm_gain, chain_entry, pool_entry, conv_taps, recur_gate, input_gate, decay_log,
    decay_shift, start_state, pool_mix, pool_scale, chain_exit, pool_exit,
):
    e = jnp.concatenate([chain_entry, pool_entry], axis=1)
    f = jnp.concatenate([chain_exit.T, pool_exit.T], axis=1)
    anywhere = pl.BlockSpec(memory_space=pl.ANY)
    vmem = pl.BlockSpec(memory_space=pltpu.VMEM)
    dma = pltpu.SemaphoreType.DMA
    return pl.pallas_call(
        kernel,
        out_shape=jax.ShapeDtypeStruct((SEQ, HALF, D), BF16),
        in_specs=[
            anywhere, vmem, anywhere, anywhere, vmem, anywhere, anywhere, vmem, anywhere, vmem,
            anywhere, vmem,
        ],
        out_specs=anywhere,
        scratch_shapes=[
            pltpu.VMEM((4, 4, 4, 32, D), BF16),
            pltpu.VMEM((4, 4, 4, 32, D), BF16),
            pltpu.VMEM((SEQ, HALO + ROWS, D), BF16),
            pltpu.VMEM((SEQ, HALO + ROWS, D), BF16),
            pltpu.VMEM((SEQ, HALO + ROWS, D), F32),
            pltpu.VMEM((SEQ, ROWS, WIDTH), F32),
            pltpu.VMEM((SEQ, ROWS, WIDTH), F32),
            pltpu.VMEM((3, CHUNK, HEAD), F32),
            pltpu.VMEM((HEADS, HEAD, HEAD), BF16),
            pltpu.VMEM((HEADS, HEAD, HEAD), BF16),
            pltpu.VMEM((HEADS, HEAD, HEAD), BF16),
            pltpu.VMEM((SEQ, ROWS, D), BF16),
            pltpu.VMEM((4, WIDTH), F32),
            pltpu.VMEM((16, 4, WIDTH), F32),
            pltpu.VMEM((SEQ, HALF, D), BF16),
            pltpu.VMEM((SEQ, HALF, D), BF16),
            pltpu.VMEM((SEQ, HALF, D), BF16),
            dma((len(ARRAYS), 3, MESSAGES)),
            dma((len(ARRAYS), 3, MESSAGES)),
            dma((7,)),
            dma((4,)),
            dma((16,)),
            dma((16,)),
            dma((8,)),
            dma((8,)),
            dma((8,)),
        ],
        compiler_params=pltpu.CompilerParams(
            collective_id=0, has_side_effects=True, vmem_limit_bytes=63 << 20
        ),
    )(
        tokens,
        norm_gain.reshape(1, D),
        e,
        f,
        conv_taps.astype(F32),
        recur_gate,
        input_gate,
        decay_log.reshape(1, WIDTH),
        decay_shift,
        start_state,
        pool_mix,
        pool_scale.reshape(1, WIDTH),
    )


def solution(mesh):
    in_specs = (
        P("fs", ("sp", "tp"), None),
        P(),
        P(("sp", "fs"), "tp"),
        P(("sp", "fs"), "tp"),
        P(None, "tp"),
        P("tp", None, None),
        P("tp", None, None),
        P("tp"),
        P("fs", "sp", "tp"),
        P("fs", "tp"),
        P("tp", None, None),
        P("tp"),
        P("tp", ("sp", "fs")),
        P("tp", ("sp", "fs")),
    )
    out_specs = P("fs", ("sp", "tp"), None)
    return jax.shard_map(
        per_device, mesh=mesh, in_specs=in_specs, out_specs=out_specs, check_vma=False
    )
```

```python
import heapq

import jax
import jax.numpy as jnp
from jax import lax
from jax.experimental import pallas as pl
from jax.experimental.pallas import tpu as pltpu
from jax.sharding import PartitionSpec as P

MESH = pl.DeviceIdType.MESH
NORM_EPSILON = 1e-06
RECUR_SCALE = 8.0
HALO = 16
ROWS = 384
HALF = ROWS // 2
HEAD = 256
HEADS = 4
WIDTH = HEADS * HEAD
D = 2048
SEQ = 2
CHUNK = 128
STRIP = 32
ALL = slice(None)
F32 = jnp.float32
BF16 = jnp.bfloat16

ORDERS = ("xyz", "yzx", "zxy")
ARRAYS = (
    (0, ((0, 384), (384, 384), (768, 256))),
    (0, ((1024, 256), (1280, 384), (1664, 384))),
    (1, ((0, 384), (384, 256), (640, 384))),
    (1, ((1024, 384), (1408, 384), (1792, 256))),
)
MESSAGES = 24


RATE, HOP, LEAD, SLACK = 46.1e3, 2.3, 1.5, 0.3


def needs(k):
    j, g = k % 4, k // 4
    if g == 0:
        return () if j < 2 else (j - 2,)
    if g == 1:
        return (0, 1, 2, 3) if j < 2 else (j + 2,)
    if j >= 2:
        return (k - 2,)
    return (0, 1, 2, 3) + ((), (4,), (5,), (6, 7))[g - 2]


def rank(m):
    a, r, k = m
    g, late = k // 4, (k % 4) // 2
    if g == 0:
        return a * 10 - 35 + 0.1 * late
    if g == 1:
        return a * 10 - 12 + late
    return a * 10 + (g - 2) + 1.5 * late


def plan():
    link, cost = {}, {}
    for a, (_, split) in enumerate(ARRAYS):
        for r in range(3):
            for k in range(MESSAGES):
                g = k // 4
                link[a, r, k] = (ORDERS[r][min(g, 2)], k % 2)
                size = (1 if g == 0 else 4) * 64 * split[r][1] / (1 + (k % 4) // 2)
                cost[a, r, k] = size / RATE
    order, arrives, free, times = [], {}, {}, [0.0]
    left = sorted(link, key=rank)
    while left:
        now = heapq.heappop(times)
        while times and times[0] <= now + 1e-5:
            heapq.heappop(times)
        here = {m for m, t in arrives.items() if t <= now + 1e-9}
        rest = []
        for m in left:
            at = free.get(link[m], 0.0)
            if not all((m[0], m[1], d) in here for d in needs(m[2])):
                rest.append(m)
            elif at - now > LEAD:
                rest.append(m)
                heapq.heappush(times, at - LEAD + 1e-5)
            else:
                free[link[m]] = max(now, at) + cost[m]
                arrives[m] = free[link[m]] + HOP
                order.append((now, m))
                heapq.heappush(times, arrives[m])
        left = rest
    done = [max(t for m, t in arrives.items() if m[0] == a) for a in range(len(ARRAYS))]
    return order, arrives, done


def minus_expm1(v):
    series = v * (1.0 / 5040.0) + (1.0 / 720.0)
    for c in (1.0 / 120.0, 1.0 / 24.0, 1.0 / 6.0, 0.5, 1.0):
        series = series * v + c
    return jnp.where(v > -0.35, -v * series, 1.0 - jnp.exp(v))


def sigmoid(v):
    return 0.5 * jnp.tanh(0.5 * v) + 0.5


def kernel(
    tok_in, gain_ref, ec_in, ep_in, f_in, taps_ref, rgate_in, igate_in, dlog_ref, shift_in, start_ref,
    mix_in, scale_ref,
    out_ref,
    E, F, X, N, CP, A, B, G, rgate, igate, mix, R, CS, CR, CT, CZ, OUTS, OUTR, OUTV,
    ssem, rsem, lsem, xsem, csend, crecv, osend, orecv, vsem,
):
    sp = lax.axis_index("sp")
    x = lax.axis_index("fs")
    c = lax.axis_index("tp")
    z = sp // 4
    y = sp % 4
    at = dict(x=x, y=y, z=z)
    after = lax.rem(sp + 1, 16)
    before = lax.rem(sp + 15, 16)

    place = {(d, by): lax.rem(at[d] + by + 4, 4) for d in "xyz" for by in (-1, 0, 1, 2)}

    def off(dim, by):
        return place[dim, by]

    def near(dim, by):
        p = dict(at)
        p[dim] = off(dim, by)
        return (p["z"] * 4 + p["y"], p["x"], c)

    own_rows = pl.ds(pl.multiple_of(HALO + c * HALF, 16), HALF)
    local = [
        pltpu.make_async_copy(src, dst, lsem.at[k])
        for k, (src, dst) in enumerate(
            (
                (ec_in, E.at[z, y, x, :, pl.ds(0, WIDTH)]),
                (tok_in, X.at[:, own_rows]),
                (f_in, F.at[z, y, x]),
                (shift_in, A),
                (rgate_in, rgate),
                (igate_in, igate),
                (mix_in, mix),
                (ep_in, E.at[z, y, x, :, pl.ds(WIDTH, WIDTH)]),
            )
        )
    ]
    for cp in local:
        cp.start()

    barrier = pltpu.get_barrier_semaphore()

    def greet(device):
        pl.semaphore_signal(barrier, inc=1, device_id=device, device_id_type=MESH)

    for by in (-1, 1):
        greet(near("x", by))
    greet((sp, x, 1 - c))
    greet((after, x, c))
    greet((before, x, c))

    def along_y(k):
        return (z * 4 + lax.rem(y + k, 4), x, c)

    def along_z(k):
        return (lax.rem(z + k, 4) * 4 + y, x, c)

    for k in range(1, 4):
        greet(along_y(k))
        greet(along_z(k))
    pl.semaphore_wait(barrier, 11)

    sent = []
    W = (E, F)

    def message(a, r, k, where, half, dim, by):
        buf, thirds = ARRAYS[a]
        lanes = pl.ds(*thirds[r])
        rows = (ALL, pl.ds(0, 16), pl.ds(16, 16))[half]
        v = W[buf].at[tuple(ALL if where[d] is None else where[d] for d in "zyx") + (rows, lanes)]
        return pltpu.make_async_remote_copy(
            src_ref=v, dst_ref=v, send_sem=ssem.at[a, r, k], recv_sem=rsem.at[a, r, k],
            device_id=near(dim, by), device_id_type=MESH,
        )

    def send(*args):
        cp = message(*args)
        cp.start()
        sent.append(args)

    def shifted(where, dim, by):
        w = dict(where)
        w[dim] = off(dim, by)
        return w

    def w1(r):
        return dict(at)

    def w2(r):
        w = dict(at)
        w[ORDERS[r][0]] = None
        return w

    def w3(r, g):
        w = w2(r)
        w[ORDERS[r][1]] = off(ORDERS[r][1], (0, -1, 1, 2)[g])
        return w

    def where_of(r, k):
        g = k // 4
        return w1(r) if g == 0 else w2(r) if g == 1 else w3(r, g - 2)

    def start(m):
        a, r, k = m
        dim = ORDERS[r][min(k // 4, 2)]
        j = k % 4
        where = where_of(r, k)
        if j >= 2:
            where = shifted(where, dim, -1 if j == 2 else 1)
        send(a, r, k, where, 0 if j < 2 else j - 1, dim, 1 if j % 2 == 0 else -1)

    def await_arrival(m):
        a, r, k = m
        dim = ORDERS[r][min(k // 4, 2)]
        j = k % 4
        by = (-1, 1, 2, 2)[j]
        message(a, r, k, shifted(where_of(r, k), dim, by), 0 if j < 2 else j - 1, dim, 1).wait_recv()

    order, arrives, done = plan()
    waited = set()
    todo = []
    for t, m in order:
        first_waits = [(m[0], m[1], d) for d in needs(m[2]) if (m[0], m[1], d) not in waited]
        waited.update(first_waits)
        todo.append((t + SLACK, first_waits, m))
    clock = [0.0]

    def perform(some):
        for _, first_waits, m in some:
            for w in first_waits:
                await_arrival(w)
            start(m)

    def due(t):
        n = 0
        while n < len(todo) and todo[n][0] <= t:
            n += 1
        some = todo[:n]
        del todo[:n]
        return some

    def until(t):
        clock[0] = max(clock[0], t)
        perform(due(clock[0]))

    def gathered(a):
        until(done[a])
        for m in sorted((m for m in arrives if m[0] == a and m not in waited), key=arrives.get):
            await_arrival(m)
            waited.add(m)

    def beside(total, each, body):
        slots = []
        for i in range(total):
            some = due(clock[0] + i * each)
            if some:
                slots.append((i, some))
        clock[0] += total * each

        def one(i, carry):
            for k, some in slots:
                pl.when(i == k)(lambda some=some: perform(some))
            body(i)
            return carry

        lax.fori_loop(0, total, one, 0)

    local[0].wait()
    local[7].wait()
    local[2].wait()
    until(SLACK)
    local[1].wait()
    tok_copy = pltpu.make_async_remote_copy(
        src_ref=X.at[:, own_rows], dst_ref=X.at[:, own_rows], send_sem=xsem.at[0],
        recv_sem=xsem.at[1], device_id=(sp, x, 1 - c), device_id_type=MESH,
    )
    tok_copy.start()
    until(5.0)
    other_rows = pl.ds(pl.multiple_of(HALO + (1 - c) * HALF, 16), HALF)
    pltpu.make_async_remote_copy(
        src_ref=X.at[:, other_rows], dst_ref=X.at[:, other_rows], send_sem=xsem.at[0],
        recv_sem=xsem.at[1], device_id=(sp, x, 1 - c), device_id_type=MESH,
    ).wait_recv()
    halo_copy = pltpu.make_async_remote_copy(
        src_ref=X.at[:, pl.ds(ROWS, HALO)], dst_ref=X.at[:, pl.ds(0, HALO)], send_sem=xsem.at[2],
        recv_sem=xsem.at[3], device_id=(after, x, c), device_id_type=MESH,
    )
    halo_copy.start()
    for k in range(3, 7):
        local[k].wait()

    first = jnp.where(sp == 0, 0.0, 1.0).astype(F32)

    def norm_tile(s, row, factor):
        v = X[s, pl.ds(row, 16), :].astype(F32)
        r = lax.rsqrt(jnp.mean(v * v, axis=-1, keepdims=True) + NORM_EPSILON)
        if factor is not None:
            r = r * factor
        N[s, pl.ds(row, 16), :] = (v * r * gain_ref[...]).astype(BF16)

    def norm_body(i):
        s = i // 24
        norm_tile(s, pl.multiple_of(HALO + (i % 24) * 16, 16), None)

    beside(48, 0.07, norm_body)
    until(11.0)
    halo_copy.wait_recv()
    for s in range(SEQ):
        norm_tile(s, 0, first)

    def entry_tile(s, col):
        cols = pl.ds(col, HEAD)
        w = E[:, :, :, :, cols].reshape(D, HEAD)
        acc = jnp.dot(N[s], w, preferred_element_type=F32)
        CP[s, :, cols] = acc.astype(BF16).astype(F32)

    def entry_body(base):
        def body(i):
            entry_tile(i % 2, pl.multiple_of(base + (i // 2) * HEAD, HEAD))
        return body

    sub = lax.broadcasted_iota(jnp.int32, (STRIP, HEAD), 0) % 8

    def gates_body(i):
        h = i // 6
        s = (i // 3) % 2
        row = pl.multiple_of((i % 3) * CHUNK, CHUNK)
        cols = pl.ds(pl.multiple_of(h * HEAD, HEAD), HEAD)
        v = CP[s, pl.ds(row, CHUNK + HALO), cols]
        taps = taps_ref[:, cols].astype(F32)
        conv = pltpu.roll(v, 3, 0) * taps[0:1]
        conv = conv + pltpu.roll(v, 2, 0) * taps[1:2]
        conv = conv + pltpu.roll(v, 1, 0) * taps[2:3]
        conv = conv + v * taps[3:4]
        conv = conv[HALO:].astype(BF16)
        G[0] = jnp.dot(conv, rgate[h], preferred_element_type=F32)
        G[1] = jnp.dot(conv, igate[h], preferred_element_type=F32)
        G[2] = conv.astype(F32)
        rate = jnp.exp(dlog_ref[:, cols]) * (-RECUR_SCALE / 6144.0)
        for k in range(CHUNK // STRIP):
            rows = pl.ds(k * STRIP, STRIP)
            to = pl.ds(pl.multiple_of(row + k * STRIP, STRIP), STRIP)
            log_decay = sigmoid(G[0, rows]) * rate + A[s, to, cols]
            a = jnp.exp(log_decay)
            b = jnp.sqrt(minus_expm1(2.0 * log_decay)) * sigmoid(G[1, rows]) * G[2, rows]
            for d in (1, 2, 4):
                keep = sub >= d
                up_a = jnp.where(keep, pltpu.roll(a, d, 0), 1.0)
                up_b = jnp.where(keep, pltpu.roll(b, d, 0), 0.0)
                b = a * up_b + b
                a = a * up_a
            A[s, to, cols] = a
            B[s, to, cols] = b

    def scan_step(t, carry):
        out = []
        rows = pl.ds(pl.multiple_of(t * 8, 8), 8)
        for s in range(SEQ):
            ha, hb = carry[2 * s], carry[2 * s + 1]
            a, b = A[s, rows, :], B[s, rows, :]
            b = a * hb + b
            a = a * ha
            A[s, rows, :] = a
            B[s, rows, :] = b
            out.append(jnp.broadcast_to(a[7:8], (8, WIDTH)))
            out.append(jnp.broadcast_to(b[7:8], (8, WIDTH)))
        return tuple(out)

    def pool_group(g, i):
        w = 2 ** (g + 1)
        s = i // 3
        row = pl.multiple_of((i % 3) * CHUNK, CHUNK)
        cols = pl.ds(WIDTH + g * HEAD, HEAD)
        v = CP[s, pl.ds(row, CHUNK + HALO), cols]
        total = v
        for d in range(g + 1):
            total = total + pltpu.roll(total, 2 ** d, 0)
        position = (sp * ROWS + row + lax.broadcasted_iota(jnp.int32, (CHUNK, HEAD), 0)).astype(F32)
        share = 1.0 / jnp.minimum(position + 1.0, float(w))
        diff = (total[HALO:] * share - v[HALO:]).astype(BF16)
        mixed = jnp.dot(diff, mix[g], preferred_element_type=F32)
        R[s, pl.ds(row, CHUNK), cols] = (mixed * scale_ref[:, pl.ds(g * HEAD, HEAD)]).astype(BF16)

    def pool_body(i):
        for g in range(HEADS):
            pool_group(g, i)

    gathered(0)
    beside(8, 0.5, entry_body(0))
    beside(24, 0.53, gates_body)
    one = jnp.ones((8, WIDTH), F32)
    nought = jnp.zeros((8, WIDTH), F32)
    ends = lax.fori_loop(0, ROWS // 8, scan_step, (one, nought, one, nought))
    until(clock[0] + 1.0)
    for s in range(SEQ):
        CS[pl.ds(s, 1), :] = ends[2 * s][0:1]
        CS[pl.ds(2 + s, 1), :] = ends[2 * s + 1][0:1]

    def carry(src, held, mine, k, device):
        base = 0 if held is CR else 4
        return pltpu.make_async_remote_copy(
            src_ref=src, dst_ref=held.at[mine], send_sem=csend.at[base + k],
            recv_sem=crecv.at[base + mine], device_id=device, device_id_type=MESH,
        )

    def to_y(k):
        return carry(CS, CR, y, k, along_y(k))

    def to_z(k):
        return carry(CT, CZ, z, k, along_z(k))

    CR[y] = CS[...]
    for k in range(1, 4):
        to_y(k).start()
    gathered(1)
    beside(8, 0.5, entry_body(WIDTH))
    for k in range(1, 4):
        carry(CS, CR, lax.rem(y + 4 - k, 4), k, along_y(k)).wait_recv()
    row_a, row_b = CR[0, 0:2, :], CR[0, 2:4, :]
    for j in range(1, 4):
        row_b = CR[j, 0:2, :] * row_b + CR[j, 2:4, :]
        row_a = CR[j, 0:2, :] * row_a
    CT[pl.ds(0, 2), :] = row_a
    CT[pl.ds(2, 2), :] = row_b
    beside(3, 0.4, pool_body)
    for k in range(1, 4):
        to_z(k).start()
    beside(3, 0.4, lambda i: pool_body(i + 3))
    for k in range(1, 4):
        carry(CT, CZ, lax.rem(z + 4 - k, 4), k, along_z(k)).wait_recv()
    h = start_ref[...]
    for j in range(3):
        h = jnp.where(j < z, CZ[j, 0:2, :] * h + CZ[j, 2:4, :], h)
    for j in range(3):
        h = jnp.where(j < y, CR[j, 0:2, :] * h + CR[j, 2:4, :], h)

    def state_body(i):
        rows = pl.ds(pl.multiple_of(i * STRIP, STRIP), STRIP)
        for s in range(SEQ):
            R[s, rows, pl.ds(0, WIDTH)] = (A[s, rows, :] * h[s:s + 1] + B[s, rows, :]).astype(BF16)

    beside(ROWS // STRIP, 0.05, state_body)
    gathered(2)

    mine = pl.ds(pl.multiple_of(c * HALF, 16), HALF)
    theirs = pl.ds(pl.multiple_of((1 - c) * HALF, 16), HALF)
    NT = (((1,), (1,)), ((), ()))

    def exit_weights(t, k0):
        return F[t // 2, pl.ds(2 * (t % 2), 2), :, :, pl.ds(k0, WIDTH)].reshape(HEAD, WIDTH)

    def chain_exit_body(t):
        cols = pl.ds(pl.multiple_of(t * HEAD, HEAD), HEAD)
        w = exit_weights(t, 0)
        for s in range(SEQ):
            CP[s, pl.ds(0, ROWS), cols] = lax.dot_general(
                R[s, :, pl.ds(0, WIDTH)], w, NT, preferred_element_type=F32
            )

    beside(8, 0.57, chain_exit_body)
    gathered(3)

    def out_copy(t):
        cols = pl.ds(pl.multiple_of(t * HEAD, HEAD), HEAD)
        return pltpu.make_async_remote_copy(
            src_ref=OUTS.at[:, :, cols], dst_ref=OUTR.at[:, :, cols], send_sem=osend.at[t],
            recv_sem=orecv.at[t], device_id=(sp, x, 1 - c), device_id_type=MESH,
        )

    def write_out(t):
        cols = pl.ds(pl.multiple_of(t * HEAD, HEAD), HEAD)
        return pltpu.make_async_copy(OUTV.at[:, :, cols], out_ref.at[:, :, cols], vsem.at[t])

    def pool_exit_body(t):
        cols = pl.ds(pl.multiple_of(t * HEAD, HEAD), HEAD)
        w = exit_weights(t, WIDTH)
        for s in range(SEQ):
            OUTS[s, :, cols] = (
                lax.dot_general(
                    R[s, theirs, pl.ds(WIDTH, WIDTH)], w, NT, preferred_element_type=F32
                )
                + CP[s, theirs, cols]
            ).astype(BF16)
        for s in range(SEQ):
            CP[s, mine, cols] += lax.dot_general(
                R[s, mine, pl.ds(WIDTH, WIDTH)], w, NT, preferred_element_type=F32
            )
        out_copy(t).start()

    def finish(t):
        cols = pl.ds(pl.multiple_of(t * HEAD, HEAD), HEAD)
        out_copy(t).wait_recv()
        for s in range(SEQ):
            OUTV[s, :, cols] = (CP[s, mine, cols] + OUTR[s, :, cols].astype(F32)).astype(BF16)
        write_out(t).start()

    def last_body(t, q):
        pool_exit_body(t)

        @pl.when(t >= 3)
        def _():
            finish(t - 3)
        return q

    lax.fori_loop(0, 8, last_body, 0)
    for t in range(5, 8):
        finish(t)

    for args in sent:
        message(*args).wait_send()
    tok_copy.wait_send()
    halo_copy.wait_send()
    for k in range(1, 4):
        to_y(k).wait_send()
        to_z(k).wait_send()
    for t in range(8):
        out_copy(t).wait_send()
        write_out(t).wait()


def per_device(
    tokens, norm_gain, chain_entry, pool_entry, conv_taps, recur_gate, input_gate, decay_log,
    decay_shift, start_state, pool_mix, pool_scale, chain_exit, pool_exit,
):
    f = jnp.concatenate([chain_exit.T, pool_exit.T], axis=1)
    anywhere = pl.BlockSpec(memory_space=pl.ANY)
    vmem = pl.BlockSpec(memory_space=pltpu.VMEM)
    dma = pltpu.SemaphoreType.DMA
    return pl.pallas_call(
        kernel,
        out_shape=jax.ShapeDtypeStruct((SEQ, HALF, D), BF16),
        in_specs=[
            anywhere, vmem, anywhere, anywhere, anywhere, vmem, anywhere, anywhere, vmem, anywhere, vmem,
            anywhere, vmem,
        ],
        out_specs=anywhere,
        scratch_shapes=[
            pltpu.VMEM((4, 4, 4, 32, D), BF16),
            pltpu.VMEM((4, 4, 4, 32, D), BF16),
            pltpu.VMEM((SEQ, HALO + ROWS, D), BF16),
            pltpu.VMEM((SEQ, HALO + ROWS, D), BF16),
            pltpu.VMEM((SEQ, HALO + ROWS, D), F32),
            pltpu.VMEM((SEQ, ROWS, WIDTH), F32),
            pltpu.VMEM((SEQ, ROWS, WIDTH), F32),
            pltpu.VMEM((3, CHUNK, HEAD), F32),
            pltpu.VMEM((HEADS, HEAD, HEAD), BF16),
            pltpu.VMEM((HEADS, HEAD, HEAD), BF16),
            pltpu.VMEM((HEADS, HEAD, HEAD), BF16),
            pltpu.VMEM((SEQ, ROWS, D), BF16),
            pltpu.VMEM((4, WIDTH), F32),
            pltpu.VMEM((4, 4, WIDTH), F32),
            pltpu.VMEM((4, WIDTH), F32),
            pltpu.VMEM((4, 4, WIDTH), F32),
            pltpu.VMEM((SEQ, HALF, D), BF16),
            pltpu.VMEM((SEQ, HALF, D), BF16),
            pltpu.VMEM((SEQ, HALF, D), BF16),
            dma((len(ARRAYS), 3, MESSAGES)),
            dma((len(ARRAYS), 3, MESSAGES)),
            dma((8,)),
            dma((4,)),
            dma((8,)),
            dma((8,)),
            dma((8,)),
            dma((8,)),
            dma((8,)),
        ],
        compiler_params=pltpu.CompilerParams(
            collective_id=0, has_side_effects=True, vmem_limit_bytes=63 << 20
        ),
    )(
        tokens,
        norm_gain.reshape(1, D),
        chain_entry,
        pool_entry,
        f,
        conv_taps,
        recur_gate,
        input_gate,
        decay_log.reshape(1, WIDTH),
        decay_shift,
        start_state,
        pool_mix,
        pool_scale.reshape(1, WIDTH),
    )


def solution(mesh):
    in_specs = (
        P("fs", ("sp", "tp"), None),
        P(),
        P(("sp", "fs"), "tp"),
        P(("sp", "fs"), "tp"),
        P(None, "tp"),
        P("tp", None, None),
        P("tp", None, None),
        P("tp"),
        P("fs", "sp", "tp"),
        P("fs", "tp"),
        P("tp", None, None),
        P("tp"),
        P("tp", ("sp", "fs")),
        P("tp", ("sp", "fs")),
    )
    out_specs = P("fs", ("sp", "tp"), None)
    return jax.shard_map(
        per_device, mesh=mesh, in_specs=in_specs, out_specs=out_specs, check_vma=False
    )
```

```python
import heapq

import jax
import jax.numpy as jnp
from jax import lax
from jax.experimental import pallas as pl
from jax.experimental.pallas import tpu as pltpu
from jax.sharding import PartitionSpec as P

MESH = pl.DeviceIdType.MESH
NORM_EPSILON = 1e-06
RECUR_SCALE = 8.0
HALO = 16
ROWS = 384
HALF = ROWS // 2
HEAD = 256
HEADS = 4
WIDTH = HEADS * HEAD
D = 2048
SEQ = 2
CHUNK = 128
STRIP = 16
ALL = slice(None)
F32 = jnp.float32
BF16 = jnp.bfloat16

ORDERS = ("xyz", "yzx", "zxy")
ARRAYS = (
    (0, ((0, 384), (384, 384), (768, 256))),
    (0, ((1024, 256), (1280, 384), (1664, 384))),
    (1, ((0, 384), (384, 256), (640, 384))),
    (1, ((1024, 384), (1408, 384), (1792, 256))),
)
MESSAGES = 24


RATE, HOP, LEAD, SLACK = 55e3, 1.8, 1.5, 0.0


def needs(k):
    j, g = k % 4, k // 4
    if g == 0:
        return () if j < 2 else (j - 2,)
    if g == 1:
        return (0, 1, 2, 3) if j < 2 else (j + 2,)
    if j >= 2:
        return (k - 2,)
    return (0, 1, 2, 3) + ((), (4,), (5,), (6, 7))[g - 2]


def rank(m):
    a, r, k = m
    g, late = k // 4, (k % 4) // 2
    if g == 0:
        return a * 10 - 35 + 0.1 * late
    if g == 1:
        return a * 10 - 12 + late
    return a * 10 + (g - 2) + 1.5 * late


def plan():
    link, cost = {}, {}
    for a, (_, split) in enumerate(ARRAYS):
        for r in range(3):
            for k in range(MESSAGES):
                g = k // 4
                link[a, r, k] = (ORDERS[r][min(g, 2)], k % 2)
                size = (1 if g == 0 else 4) * 64 * split[r][1] / (1 + (k % 4) // 2)
                cost[a, r, k] = size / RATE
    order, arrives, free, times = [], {}, {}, [0.0]
    left = sorted(link, key=rank)
    while left:
        now = heapq.heappop(times)
        while times and times[0] <= now + 1e-5:
            heapq.heappop(times)
        here = {m for m, t in arrives.items() if t <= now + 1e-9}
        rest = []
        for m in left:
            at = free.get(link[m], 0.0)
            if not all((m[0], m[1], d) in here for d in needs(m[2])):
                rest.append(m)
            elif at - now > LEAD:
                rest.append(m)
                heapq.heappush(times, at - LEAD + 1e-5)
            else:
                free[link[m]] = max(now, at) + cost[m]
                arrives[m] = free[link[m]] + HOP
                order.append((now, m))
                heapq.heappush(times, arrives[m])
        left = rest
    done = [max(t for m, t in arrives.items() if m[0] == a) for a in range(len(ARRAYS))]
    return order, arrives, done


def minus_expm1(v):
    series = v * (1.0 / 5040.0) + (1.0 / 720.0)
    for c in (1.0 / 120.0, 1.0 / 24.0, 1.0 / 6.0, 0.5, 1.0):
        series = series * v + c
    return jnp.where(v > -0.35, -v * series, 1.0 - jnp.exp(v))


def sigmoid(v):
    return 0.5 * jnp.tanh(0.5 * v) + 0.5


def kernel(
    tok_in, gain_ref, ec_in, ep_in, f_in, taps_ref, rgate_in, igate_in, dlog_ref, shift_in, start_ref,
    mix_in, scale_ref,
    out_ref,
    E, F, X, N, CP, A, B, G, rgate, igate, mix, R, CS, CR, CT, CZ, OUTS, OUTR, OUTV,
    ssem, rsem, lsem, xsem, csend, crecv, osend, orecv, vsem,
):
    sp = lax.axis_index("sp")
    x = lax.axis_index("fs")
    c = lax.axis_index("tp")
    z = sp // 4
    y = sp % 4
    at = dict(x=x, y=y, z=z)
    after = lax.rem(sp + 1, 16)
    before = lax.rem(sp + 15, 16)

    place = {(d, by): lax.rem(at[d] + by + 4, 4) for d in "xyz" for by in (-1, 0, 1, 2)}

    def off(dim, by):
        return place[dim, by]

    def near(dim, by):
        p = dict(at)
        p[dim] = off(dim, by)
        return (p["z"] * 4 + p["y"], p["x"], c)

    own_rows = pl.ds(pl.multiple_of(HALO + c * HALF, 16), HALF)
    local = [
        pltpu.make_async_copy(src, dst, lsem.at[k])
        for k, (src, dst) in enumerate(
            (
                (ec_in, E.at[z, y, x, :, pl.ds(0, WIDTH)]),
                (tok_in, X.at[:, own_rows]),
                (f_in, F.at[z, y, x]),
                (shift_in, A),
                (rgate_in, rgate),
                (igate_in, igate),
                (mix_in, mix),
                (ep_in, E.at[z, y, x, :, pl.ds(WIDTH, WIDTH)]),
            )
        )
    ]
    for cp in local:
        cp.start()

    barrier = pltpu.get_barrier_semaphore()

    def greet(device):
        pl.semaphore_signal(barrier, inc=1, device_id=device, device_id_type=MESH)

    for by in (-1, 1):
        greet(near("x", by))
    greet((sp, x, 1 - c))
    greet((after, x, c))
    greet((before, x, c))

    def along_y(k):
        return (z * 4 + lax.rem(y + k, 4), x, c)

    def along_z(k):
        return (lax.rem(z + k, 4) * 4 + y, x, c)

    for k in range(1, 4):
        greet(along_y(k))
        greet(along_z(k))
    pl.semaphore_wait(barrier, 11)

    sent = []
    W = (E, F)

    def message(a, r, k, where, half, dim, by):
        buf, thirds = ARRAYS[a]
        lanes = pl.ds(*thirds[r])
        rows = (ALL, pl.ds(0, 16), pl.ds(16, 16))[half]
        v = W[buf].at[tuple(ALL if where[d] is None else where[d] for d in "zyx") + (rows, lanes)]
        return pltpu.make_async_remote_copy(
            src_ref=v, dst_ref=v, send_sem=ssem.at[a, r, k], recv_sem=rsem.at[a, r, k],
            device_id=near(dim, by), device_id_type=MESH,
        )

    def send(*args):
        cp = message(*args)
        cp.start()
        sent.append(args)

    def shifted(where, dim, by):
        w = dict(where)
        w[dim] = off(dim, by)
        return w

    def w1(r):
        return dict(at)

    def w2(r):
        w = dict(at)
        w[ORDERS[r][0]] = None
        return w

    def w3(r, g):
        w = w2(r)
        w[ORDERS[r][1]] = off(ORDERS[r][1], (0, -1, 1, 2)[g])
        return w

    def where_of(r, k):
        g = k // 4
        return w1(r) if g == 0 else w2(r) if g == 1 else w3(r, g - 2)

    def start(m):
        a, r, k = m
        dim = ORDERS[r][min(k // 4, 2)]
        j = k % 4
        where = where_of(r, k)
        if j >= 2:
            where = shifted(where, dim, -1 if j == 2 else 1)
        send(a, r, k, where, 0 if j < 2 else j - 1, dim, 1 if j % 2 == 0 else -1)

    def await_arrival(m):
        a, r, k = m
        dim = ORDERS[r][min(k // 4, 2)]
        j = k % 4
        by = (-1, 1, 2, 2)[j]
        message(a, r, k, shifted(where_of(r, k), dim, by), 0 if j < 2 else j - 1, dim, 1).wait_recv()

    order, arrives, done = plan()
    waited = set()
    todo = []
    for t, m in order:
        first_waits = [(m[0], m[1], d) for d in needs(m[2]) if (m[0], m[1], d) not in waited]
        waited.update(first_waits)
        todo.append((t + SLACK, first_waits, m))
    clock = [0.0]

    def perform(some):
        for _, first_waits, m in some:
            for w in first_waits:
                await_arrival(w)
            start(m)

    def due(t):
        n = 0
        while n < len(todo) and todo[n][0] <= t:
            n += 1
        some = todo[:n]
        del todo[:n]
        return some

    def until(t):
        clock[0] = max(clock[0], t)
        perform(due(clock[0]))

    when = {m: t for t, m in order}
    settled = set()

    def settle(t):
        for args in sent:
            if args[:3] not in settled and when[args[:3]] <= t:
                message(*args).wait_send()
                settled.add(args[:3])

    def gathered(a):
        until(done[a])
        settle(done[a] - 8.0)
        for m in sorted((m for m in arrives if m[0] == a and m not in waited), key=arrives.get):
            await_arrival(m)
            waited.add(m)

    def beside(total, each, body):
        slots = []
        for i in range(total):
            some = due(clock[0] + i * each)
            if some:
                slots.append((i, some))
        clock[0] += total * each

        def one(i, carry):
            for k, some in slots:
                pl.when(i == k)(lambda some=some: perform(some))
            body(i)
            return carry

        lax.fori_loop(0, total, one, 0)

    local[0].wait()
    local[7].wait()
    local[2].wait()
    until(SLACK)
    local[1].wait()
    tok_copy = pltpu.make_async_remote_copy(
        src_ref=X.at[:, own_rows], dst_ref=X.at[:, own_rows], send_sem=xsem.at[0],
        recv_sem=xsem.at[1], device_id=(sp, x, 1 - c), device_id_type=MESH,
    )
    tok_copy.start()
    until(5.0)
    other_rows = pl.ds(pl.multiple_of(HALO + (1 - c) * HALF, 16), HALF)
    pltpu.make_async_remote_copy(
        src_ref=X.at[:, other_rows], dst_ref=X.at[:, other_rows], send_sem=xsem.at[0],
        recv_sem=xsem.at[1], device_id=(sp, x, 1 - c), device_id_type=MESH,
    ).wait_recv()
    halo_copy = pltpu.make_async_remote_copy(
        src_ref=X.at[:, pl.ds(ROWS, HALO)], dst_ref=X.at[:, pl.ds(0, HALO)], send_sem=xsem.at[2],
        recv_sem=xsem.at[3], device_id=(after, x, c), device_id_type=MESH,
    )
    halo_copy.start()
    for k in range(3, 7):
        local[k].wait()

    first = jnp.where(sp == 0, 0.0, 1.0).astype(F32)

    def norm_tile(s, row, factor):
        v = X[s, pl.ds(row, 16), :].astype(F32)
        r = lax.rsqrt(jnp.mean(v * v, axis=-1, keepdims=True) + NORM_EPSILON)
        if factor is not None:
            r = r * factor
        N[s, pl.ds(row, 16), :] = (v * r * gain_ref[...]).astype(BF16)

    def norm_body(i):
        s = i // 24
        norm_tile(s, pl.multiple_of(HALO + (i % 24) * 16, 16), None)

    beside(48, 0.07, norm_body)
    until(11.0)
    halo_copy.wait_recv()
    for s in range(SEQ):
        norm_tile(s, 0, first)

    def entry_tile(s, col):
        cols = pl.ds(col, HEAD)
        w = E[:, :, :, :, cols].reshape(D, HEAD)
        acc = jnp.dot(N[s], w, preferred_element_type=F32)
        CP[s, :, cols] = acc.astype(BF16).astype(F32)

    def entry_body(base):
        def body(i):
            entry_tile(i % 2, pl.multiple_of(base + (i // 2) * HEAD, HEAD))
        return body

    sub = lax.broadcasted_iota(jnp.int32, (STRIP, HEAD), 0) % 8

    def gates_body(i):
        h = i // 6
        s = (i // 3) % 2
        row = pl.multiple_of((i % 3) * CHUNK, CHUNK)
        cols = pl.ds(pl.multiple_of(h * HEAD, HEAD), HEAD)
        v = CP[s, pl.ds(row, CHUNK + HALO), cols]
        taps = taps_ref[:, cols].astype(F32)
        conv = pltpu.roll(v, 3, 0) * taps[0:1]
        conv = conv + pltpu.roll(v, 2, 0) * taps[1:2]
        conv = conv + pltpu.roll(v, 1, 0) * taps[2:3]
        conv = conv + v * taps[3:4]
        conv = conv[HALO:].astype(BF16)
        G[0] = jnp.dot(conv, rgate[h], preferred_element_type=F32)
        G[1] = jnp.dot(conv, igate[h], preferred_element_type=F32)
        G[2] = conv.astype(F32)
        rate = jnp.exp(dlog_ref[:, cols]) * (-RECUR_SCALE / 6144.0)
        for k in range(CHUNK // STRIP):
            rows = pl.ds(k * STRIP, STRIP)
            to = pl.ds(pl.multiple_of(row + k * STRIP, STRIP), STRIP)
            log_decay = sigmoid(G[0, rows]) * rate + A[s, to, cols]
            a = jnp.exp(log_decay)
            b = jnp.sqrt(minus_expm1(2.0 * log_decay)) * sigmoid(G[1, rows]) * G[2, rows]
            for d in (1, 2, 4):
                keep = sub >= d
                up_a = jnp.where(keep, pltpu.roll(a, d, 0), 1.0)
                up_b = jnp.where(keep, pltpu.roll(b, d, 0), 0.0)
                b = a * up_b + b
                a = a * up_a
            A[s, to, cols] = a
            B[s, to, cols] = b

    def scan_step(t, carry):
        out = []
        rows = pl.ds(pl.multiple_of(t * 8, 8), 8)
        for s in range(SEQ):
            ha, hb = carry[2 * s], carry[2 * s + 1]
            a, b = A[s, rows, :], B[s, rows, :]
            b = a * hb + b
            a = a * ha
            A[s, rows, :] = a
            B[s, rows, :] = b
            out.append(jnp.broadcast_to(a[7:8], (8, WIDTH)))
            out.append(jnp.broadcast_to(b[7:8], (8, WIDTH)))
        return tuple(out)

    def pool_group(g, i):
        w = 2 ** (g + 1)
        s = i // 3
        row = pl.multiple_of((i % 3) * CHUNK, CHUNK)
        cols = pl.ds(WIDTH + g * HEAD, HEAD)
        v = CP[s, pl.ds(row, CHUNK + HALO), cols]
        total = v
        for d in range(g + 1):
            total = total + pltpu.roll(total, 2 ** d, 0)
        position = (sp * ROWS + row + lax.broadcasted_iota(jnp.int32, (CHUNK, HEAD), 0)).astype(F32)
        share = 1.0 / jnp.minimum(position + 1.0, float(w))
        diff = (total[HALO:] * share - v[HALO:]).astype(BF16)
        mixed = jnp.dot(diff, mix[g], preferred_element_type=F32)
        R[s, pl.ds(row, CHUNK), cols] = (mixed * scale_ref[:, pl.ds(g * HEAD, HEAD)]).astype(BF16)

    def pool_body(i):
        for g in range(HEADS):
            pool_group(g, i)

    gathered(0)
    beside(8, 0.5, entry_body(0))
    beside(24, 0.53, gates_body)
    one = jnp.ones((8, WIDTH), F32)
    nought = jnp.zeros((8, WIDTH), F32)
    ends = lax.fori_loop(0, ROWS // 8, scan_step, (one, nought, one, nought))
    until(clock[0] + 1.0)
    for s in range(SEQ):
        CS[pl.ds(s, 1), :] = ends[2 * s][0:1]
        CS[pl.ds(2 + s, 1), :] = ends[2 * s + 1][0:1]

    def carry(src, held, mine, k, device):
        base = 0 if held is CR else 4
        return pltpu.make_async_remote_copy(
            src_ref=src, dst_ref=held.at[mine], send_sem=csend.at[base + k],
            recv_sem=crecv.at[base + mine], device_id=device, device_id_type=MESH,
        )

    def to_y(k):
        return carry(CS, CR, y, k, along_y(k))

    def to_z(k):
        return carry(CT, CZ, z, k, along_z(k))

    CR[y] = CS[...]
    for k in range(1, 4):
        to_y(k).start()
    gathered(1)
    beside(8, 0.5, entry_body(WIDTH))
    for k in range(1, 4):
        carry(CS, CR, lax.rem(y + 4 - k, 4), k, along_y(k)).wait_recv()
    row_a, row_b = CR[0, 0:2, :], CR[0, 2:4, :]
    for j in range(1, 4):
        row_b = CR[j, 0:2, :] * row_b + CR[j, 2:4, :]
        row_a = CR[j, 0:2, :] * row_a
    CT[pl.ds(0, 2), :] = row_a
    CT[pl.ds(2, 2), :] = row_b
    beside(3, 0.4, pool_body)
    for k in range(1, 4):
        to_z(k).start()
    beside(3, 0.4, lambda i: pool_body(i + 3))
    for k in range(1, 4):
        carry(CT, CZ, lax.rem(z + 4 - k, 4), k, along_z(k)).wait_recv()
    h = start_ref[...]
    for j in range(3):
        h = jnp.where(j < z, CZ[j, 0:2, :] * h + CZ[j, 2:4, :], h)
    for j in range(3):
        h = jnp.where(j < y, CR[j, 0:2, :] * h + CR[j, 2:4, :], h)

    def state_body(i):
        rows = pl.ds(pl.multiple_of(i * STRIP, STRIP), STRIP)
        for s in range(SEQ):
            R[s, rows, pl.ds(0, WIDTH)] = (A[s, rows, :] * h[s:s + 1] + B[s, rows, :]).astype(BF16)

    beside(ROWS // STRIP, 0.05, state_body)
    gathered(2)

    mine = pl.ds(pl.multiple_of(c * HALF, 16), HALF)
    theirs = pl.ds(pl.multiple_of((1 - c) * HALF, 16), HALF)
    NT = (((1,), (1,)), ((), ()))

    def exit_weights(t, k0):
        return F[t // 2, pl.ds(2 * (t % 2), 2), :, :, pl.ds(k0, WIDTH)].reshape(HEAD, WIDTH)

    def chain_exit_body(t):
        cols = pl.ds(pl.multiple_of(t * HEAD, HEAD), HEAD)
        w = exit_weights(t, 0)
        for s in range(SEQ):
            CP[s, pl.ds(0, ROWS), cols] = lax.dot_general(
                R[s, :, pl.ds(0, WIDTH)], w, NT, preferred_element_type=F32
            )

    beside(8, 0.57, chain_exit_body)
    gathered(3)

    def out_copy(t):
        cols = pl.ds(pl.multiple_of(t * HEAD, HEAD), HEAD)
        return pltpu.make_async_remote_copy(
            src_ref=OUTS.at[:, :, cols], dst_ref=OUTR.at[:, :, cols], send_sem=osend.at[t],
            recv_sem=orecv.at[t], device_id=(sp, x, 1 - c), device_id_type=MESH,
        )

    def write_out(t):
        cols = pl.ds(pl.multiple_of(t * HEAD, HEAD), HEAD)
        return pltpu.make_async_copy(OUTV.at[:, :, cols], out_ref.at[:, :, cols], vsem.at[t])

    def pool_exit_body(t):
        cols = pl.ds(pl.multiple_of(t * HEAD, HEAD), HEAD)
        w = exit_weights(t, WIDTH)
        for s in range(SEQ):
            OUTS[s, :, cols] = (
                lax.dot_general(
                    R[s, theirs, pl.ds(WIDTH, WIDTH)], w, NT, preferred_element_type=F32
                )
                + CP[s, theirs, cols]
            ).astype(BF16)
        for s in range(SEQ):
            CP[s, mine, cols] += lax.dot_general(
                R[s, mine, pl.ds(WIDTH, WIDTH)], w, NT, preferred_element_type=F32
            )
        out_copy(t).start()

    def finish(t):
        cols = pl.ds(pl.multiple_of(t * HEAD, HEAD), HEAD)
        out_copy(t).wait_recv()
        for s in range(SEQ):
            OUTV[s, :, cols] = (CP[s, mine, cols] + OUTR[s, :, cols].astype(F32)).astype(BF16)
        write_out(t).start()

    def last_body(t, q):
        pool_exit_body(t)

        @pl.when(t >= 3)
        def _():
            finish(t - 3)
        return q

    lax.fori_loop(0, 8, last_body, 0)
    for t in range(5, 8):
        finish(t)

    settle(1e9)
    tok_copy.wait_send()
    halo_copy.wait_send()
    for k in range(1, 4):
        to_y(k).wait_send()
        to_z(k).wait_send()
    for t in range(8):
        out_copy(t).wait_send()
        write_out(t).wait()


def per_device(
    tokens, norm_gain, chain_entry, pool_entry, conv_taps, recur_gate, input_gate, decay_log,
    decay_shift, start_state, pool_mix, pool_scale, chain_exit, pool_exit,
):
    f = jnp.concatenate([chain_exit.T, pool_exit.T], axis=1)
    anywhere = pl.BlockSpec(memory_space=pl.ANY)
    vmem = pl.BlockSpec(memory_space=pltpu.VMEM)
    dma = pltpu.SemaphoreType.DMA
    return pl.pallas_call(
        kernel,
        out_shape=jax.ShapeDtypeStruct((SEQ, HALF, D), BF16),
        in_specs=[
            anywhere, vmem, anywhere, anywhere, anywhere, vmem, anywhere, anywhere, vmem, anywhere, vmem,
            anywhere, vmem,
        ],
        out_specs=anywhere,
        scratch_shapes=[
            pltpu.VMEM((4, 4, 4, 32, D), BF16),
            pltpu.VMEM((4, 4, 4, 32, D), BF16),
            pltpu.VMEM((SEQ, HALO + ROWS, D), BF16),
            pltpu.VMEM((SEQ, HALO + ROWS, D), BF16),
            pltpu.VMEM((SEQ, HALO + ROWS, D), F32),
            pltpu.VMEM((SEQ, ROWS, WIDTH), F32),
            pltpu.VMEM((SEQ, ROWS, WIDTH), F32),
            pltpu.VMEM((3, CHUNK, HEAD), F32),
            pltpu.VMEM((HEADS, HEAD, HEAD), BF16),
            pltpu.VMEM((HEADS, HEAD, HEAD), BF16),
            pltpu.VMEM((HEADS, HEAD, HEAD), BF16),
            pltpu.VMEM((SEQ, ROWS, D), BF16),
            pltpu.VMEM((4, WIDTH), F32),
            pltpu.VMEM((4, 4, WIDTH), F32),
            pltpu.VMEM((4, WIDTH), F32),
            pltpu.VMEM((4, 4, WIDTH), F32),
            pltpu.VMEM((SEQ, HALF, D), BF16),
            pltpu.VMEM((SEQ, HALF, D), BF16),
            pltpu.VMEM((SEQ, HALF, D), BF16),
            dma((len(ARRAYS), 3, MESSAGES)),
            dma((len(ARRAYS), 3, MESSAGES)),
            dma((8,)),
            dma((4,)),
            dma((8,)),
            dma((8,)),
            dma((8,)),
            dma((8,)),
            dma((8,)),
        ],
        compiler_params=pltpu.CompilerParams(
            collective_id=0, has_side_effects=True, vmem_limit_bytes=63 << 20
        ),
    )(
        tokens,
        norm_gain.reshape(1, D),
        chain_entry,
        pool_entry,
        f,
        conv_taps,
        recur_gate,
        input_gate,
        decay_log.reshape(1, WIDTH),
        decay_shift,
        start_state,
        pool_mix,
        pool_scale.reshape(1, WIDTH),
    )


def solution(mesh):
    in_specs = (
        P("fs", ("sp", "tp"), None),
        P(),
        P(("sp", "fs"), "tp"),
        P(("sp", "fs"), "tp"),
        P(None, "tp"),
        P("tp", None, None),
        P("tp", None, None),
        P("tp"),
        P("fs", "sp", "tp"),
        P("fs", "tp"),
        P("tp", None, None),
        P("tp"),
        P("tp", ("sp", "fs")),
        P("tp", ("sp", "fs")),
    )
    out_specs = P("fs", ("sp", "tp"), None)
    return jax.shard_map(
        per_device, mesh=mesh, in_specs=in_specs, out_specs=out_specs, check_vma=False
    )
```
